128 devices in a mesh: fs: 16 (over z, x), rep: 4 (over y), tp: 2 (over core).
Axes of the slice: x: 4, y: 4, z: 4, core: 2. Of those that a mesh axis runs over, the one named last changes fastest.
Arguments:
- saved_query: bfloat16 [196608, 512], P(('fs', 'rep')), may hold values from -30 to 30
- upstream_query: bfloat16 [196608, 1536], P(('fs', 'rep'), 'tp'), may hold values from -0.067658235 to 0.067658235
- weight_query: float32 [512, 1536], P('fs', 'tp'), may hold values from -0.25 to 0.25
- moment_query: float32 [512, 1536], P('fs', 'tp'), may hold values from -12 to 12
- left_query: bfloat16 [512, 512], P('fs'), may hold values from -2 to 2
- right_query: bfloat16 [4, 384, 384], P('tp'), may hold values from -2 to 2
- saved_output: bfloat16 [196608, 1024], P(('fs', 'rep')), may hold values from -30 to 30
- upstream_output: bfloat16 [196608, 2048], P(('fs', 'rep'), 'tp'), may hold values from -0.067658235 to 0.067658235
- weight_output: float32 [1024, 2048], P('fs', 'tp'), may hold values from -0.1875 to 0.1875
- moment_output: float32 [1024, 2048], P('fs', 'tp'), may hold values from -12 to 12
- left_output: bfloat16 [1024, 1024], P('fs'), may hold values from -2 to 2
- right_output: bfloat16 [4, 512, 512], P('tp'), may hold values from -2 to 2
Outputs:
- new_weight_query: float32 [512, 1536], P('fs', 'tp')
- new_moment_query: float32 [512, 1536], P('fs', 'tp')
- copy_query: bfloat16 [512, 1536], P(None, 'tp')
- new_weight_output: float32 [1024, 2048], P('fs', 'tp')
- new_moment_output: float32 [1024, 2048], P('fs', 'tp')
- copy_output: bfloat16 [1024, 2048], P(None, 'tp')
The draws below stay inside these ranges and needn't reach their ends.
All inputs are finite; a program needn't handle non-finite values.
Results may differ from the reference program's by a relative error of at most 0.0085.
Values may be sent and summed in bfloat16 or wider, within the bound.
No kernel may reach another device: no remote copies, remote signals or barrier semaphores. Data moves between devices by JAX's collectives and lax.ppermute only.
A program may use at most 128 MiB of HBM per device.

```python
import jax
import jax.numpy as jnp
from jax import lax

QL = 512
QCOLS = 1536
VW = 1024
DM = 2048
QBLK = 384
OBLK = 512
TOKENS = 196608


def scaled_normal(key, rows, cols, unit):
    first, second = jax.random.split(key, 2)
    ramp = 3.0 ** (jnp.arange(cols, dtype=jnp.float32) / cols)
    rough = jnp.exp(jax.random.uniform(second, (cols,), jnp.float32, -0.5, 0.5))
    base = jnp.clip(jax.random.normal(first, (rows, cols), jnp.float32), -6.0, 6.0)
    return (base * ramp * rough * unit).astype(jnp.bfloat16)


def root_factor(key, count, size):
    first, second = jax.random.split(key)
    diag = jax.random.uniform(first, (count, size), jnp.float32, 0.6, 1.4)
    off = jnp.clip(jax.random.normal(second, (count, size, size), jnp.float32), -4.0, 4.0)
    off = off * (0.6 / size ** 0.5)
    off = 0.5 * (off + jnp.swapaxes(off, 1, 2))
    eye = jnp.eye(size, dtype=jnp.float32)
    return (off * (1.0 - eye) + diag[:, :, None] * eye).astype(jnp.bfloat16)


def draw_saved_query(key, part):
    return scaled_normal(jax.random.fold_in(key, 11), TOKENS, QL, 1.0)


def draw_upstream_query(key, part):
    return scaled_normal(jax.random.fold_in(key, 12), TOKENS, QCOLS, TOKENS ** (-0.5))


def draw_left_query(key, part):
    return root_factor(jax.random.fold_in(key, 13), 1, QL)[0]


def draw_right_query(key, part):
    return root_factor(jax.random.fold_in(key, 14), QCOLS // QBLK, QBLK)


def draw_saved_output(key, part):
    return scaled_normal(jax.random.fold_in(key, 21), TOKENS, VW, 1.0)


def draw_upstream_output(key, part):
    return scaled_normal(jax.random.fold_in(key, 22), TOKENS, DM, TOKENS ** (-0.5))


def draw_left_output(key, part):
    return root_factor(jax.random.fold_in(key, 23), 1, VW)[0]


def draw_right_output(key, part):
    return root_factor(jax.random.fold_in(key, 24), DM // OBLK, OBLK)


def level_of(key, shape, cuts, smallest, largest):
    level, own = 1.0, jax.random.fold_in(key, 6)
    for axis_at, shards_of in cuts:
        steps = jnp.exp(jax.random.uniform(jax.random.fold_in(own, axis_at), (shards_of,), jnp.float32, smallest / len(cuts), largest / len(cuts)))
        level = level * jnp.repeat(steps, shape[axis_at] // shards_of).reshape([-1 if axis == axis_at else 1 for axis in range(len(shape))])
    return level


def bell_draw(rng, extent, scale, bound, cuts=(), held_as=jnp.bfloat16):
    values = jax.random.normal(rng, extent, jnp.float32) * scale
    if len(cuts) > 0:
        values = level_of(rng, extent, cuts, -0.22, 0.18) * values
    return jnp.clip(values, min=-bound, max=bound).astype(held_as)


def setup_inputs(seed: int = 0) -> dict:
    splits = jax.random.split(jax.random.key(seed), 13)
    return {
        "saved_query": draw_saved_query(jax.random.fold_in(splits[12], 71), 0),
        "upstream_query": draw_upstream_query(jax.random.fold_in(splits[12], 71), 0),
        "weight_query": bell_draw(splits[2], (QL, QCOLS), QL ** -0.5, 0.25, ((0, 16), (1, 2)), jnp.float32),
        "moment_query": bell_draw(splits[3], (QL, QCOLS), 2.0, 12.0, ((0, 16), (1, 2)), jnp.float32),
        "left_query": draw_left_query(jax.random.fold_in(splits[12], 71), 0),
        "right_query": draw_right_query(jax.random.fold_in(splits[12], 71), 0),
        "saved_output": draw_saved_output(jax.random.fold_in(splits[12], 71), 0),
        "upstream_output": draw_upstream_output(jax.random.fold_in(splits[12], 71), 0),
        "weight_output": bell_draw(splits[8], (VW, DM), VW ** -0.5, 0.1875, ((0, 16), (1, 2)), jnp.float32),
        "moment_output": bell_draw(splits[9], (VW, DM), 2.0, 12.0, ((0, 16), (1, 2)), jnp.float32),
        "left_output": draw_left_output(jax.random.fold_in(splits[12], 71), 0),
        "right_output": draw_right_output(jax.random.fold_in(splits[12], 71), 0),
    }


def precondition(saved, upstream, left, right, block):
    grad = lax.dot_general(saved, upstream, (((0,), (0,)), ((), ())), preferred_element_type=jnp.float32)
    rounded = grad.astype(jnp.bfloat16)
    left_prod = jnp.dot(left, rounded, preferred_element_type=jnp.float32).astype(jnp.bfloat16)
    rows = left_prod.shape[0]
    shaped = left_prod.reshape(rows, -1, block).astype(jnp.float32)
    direction = jnp.einsum('rnb,nbc->rnc', shaped, right.astype(jnp.float32)).reshape(rows, -1)
    return (grad, direction)

def finish(weight, moment, direction, scale):
    new_moment = 0.8 * moment + scale * direction
    new_weight = 0.998 * weight - 0.02 * new_moment
    return (new_weight, new_moment, new_weight.astype(jnp.bfloat16))

def reference(saved_query, upstream_query, weight_query, moment_query, left_query, right_query, saved_output, upstream_output, weight_output, moment_output, left_output, right_output):
    grad_q, dir_q = precondition(saved_query, upstream_query, left_query, right_query, QBLK)
    grad_o, dir_o = precondition(saved_output, upstream_output, left_output, right_output, OBLK)
    scale_q = jnp.sqrt(jnp.sum(grad_q * grad_q) / (jnp.sum(dir_q * dir_q) + 1e-06))
    scale_o = jnp.sqrt(jnp.sum(grad_o * grad_o) / (jnp.sum(dir_o * dir_o) + 1e-06))
    wq, mq, cq = finish(weight_query, moment_query, dir_q, scale_q)
    wo, mo, co = finish(weight_output, moment_output, dir_o, scale_o)
    return (wq, mq, cq, wo, mo, co)
```

```python
import jax
import jax.numpy as jnp
from jax import lax
from jax.sharding import Mesh, PartitionSpec as P

AXES = ("z", "x", "y", "tp")
F32 = jnp.float32
BF16 = jnp.bfloat16


def shift_pairs(dims, k):
    pairs = []
    for z in range(4):
        for x in range(4):
            for y in range(4):
                for t in range(2):
                    at = {"z": z, "x": x, "y": y}
                    at[dims[t]] = (at[dims[t]] + k) % 4
                    there = ((at["z"] * 4 + at["x"]) * 4 + at["y"]) * 2 + t
                    pairs.append((((z * 4 + x) * 4 + y) * 2 + t, there))
    return pairs


def shifted(array, dims, k):
    return lax.ppermute(array, AXES, shift_pairs(dims, k))


def other_core(array):
    return lax.ppermute(array, "tp", [(0, 1), (1, 0)])


def place_on(dims):
    t = lax.axis_index("tp")
    return jnp.where(t == 0, lax.axis_index(dims[0]), lax.axis_index(dims[1]))


def summed(own, first, second, third):
    f = lambda v: v.astype(F32)
    return (f(own) + f(second)) + (f(first) + f(third))


def scatter_sum(part, dims):
    me = place_on(dims)
    width = part.shape[1] // 4
    block = lambda k: lax.dynamic_slice_in_dim(part, (me + k) % 4 * width, width, 1)
    got = [shifted(block(k), dims, k) for k in (1, 2, 3)]
    return summed(block(0), *got)


def all_sum(value, dims):
    sent = value.astype(BF16)
    return summed(sent, *[shifted(sent, dims, k) for k in (1, 2, 3)])


def in_place(pieces, me):
    stacked = jnp.stack(pieces)
    return [lax.dynamic_index_in_dim(stacked, (me - a) % 4, 0, False) for a in range(4)]


def gather_rows(array):
    first = [array] + [shifted(array, ("x", "z"), k) for k in (1, 2, 3)]
    block = jnp.stack(in_place(first, place_on(("x", "z"))))
    second = [block] + [shifted(block, ("z", "x"), k) for k in (1, 2, 3)]
    full = jnp.stack(in_place(second, place_on(("z", "x"))))
    return jnp.where(lax.axis_index("tp") == 0, full, jnp.swapaxes(full, 0, 1))


def partial_grad(saved, upstream):
    return lax.dot_general(
        saved, upstream, (((0,), (0,)), ((), ())), preferred_element_type=F32
    ).astype(BF16)


def left_quarter(grad, left):
    grad_sq = jnp.sum(grad * grad)
    prod = jnp.dot(left, grad.astype(BF16), preferred_element_type=F32).astype(BF16)
    high = lax.reduce_precision(grad_sq, 8, 7)
    low = grad_sq - high
    tail = jnp.concatenate(
        [jnp.full((8, prod.shape[1]), high, BF16), jnp.full((8, prod.shape[1]), low, BF16)]
    )
    return jnp.concatenate([prod, tail])


def gather_quarters(packed, dims):
    pieces = [packed] + [shifted(packed, dims, k) for k in (1, 2, 3)]
    rows = packed.shape[0] - 16
    sums = [p[rows, 0].astype(F32) + p[rows + 8, 0].astype(F32) for p in pieces]
    blocks = in_place(pieces, place_on(dims))
    return (sums[0] + sums[2]) + (sums[1] + sums[3]), jnp.concatenate(
        [b[:rows] for b in blocks], axis=1
    )


def direction_of(prod, right):
    width = right.shape[1]
    return jnp.concatenate(
        [
            jnp.dot(prod[:, n * width : (n + 1) * width], right[n], preferred_element_type=F32)
            for n in range(right.shape[0])
        ],
        axis=1,
    )


Q_DIMS = (("x", "x"), ("y", "y"), ("z", "z"))
O_DIMS = (("y", "z"), ("z", "x"), ("x", "y"))


def local(sq, uq, wq, mq, lq, rq, so, uo, wo, mo, lo, ro):
    t = lax.axis_index("tp")
    fs = lax.axis_index("z") * 4 + lax.axis_index("x")
    half = lambda a: lax.dynamic_slice_in_dim(a, t * (a.shape[0] // 2), a.shape[0] // 2, 0)
    base_q = 0.998 * wq - 0.016 * mq
    base_o = 0.998 * wo - 0.016 * mo
    left_part = jnp.concatenate([half(lo), half(lq).reshape(8, 1024)])
    base_part = jnp.concatenate([base_o.astype(BF16), base_q.astype(BF16).reshape(24, 1024)])

    part_o = partial_grad(so, uo)
    part_q = partial_grad(sq, uq)
    left_all = gather_rows(left_part)
    left_else = other_core(left_all)
    left_both = jnp.where(
        t == 0, jnp.stack([left_all, left_else], 2), jnp.stack([left_else, left_all], 2)
    )
    left_o = left_both[:, :, :, :32].reshape(1024, 1024)
    left_q = left_both[:, :, :, 32:].reshape(512, 512)
    base_all = gather_rows(base_part)
    base_all_o = base_all[:, :, :64].reshape(1024, 1024)
    base_all_q = base_all[:, :, 64:].reshape(512, 768)

    grad_o = scatter_sum(part_o, O_DIMS[0])
    grad_q = scatter_sum(part_q, Q_DIMS[0])
    for o_dims, q_dims in zip(O_DIMS[1:], Q_DIMS[1:]):
        grad_o = all_sum(grad_o, o_dims)
        grad_q = all_sum(grad_q, q_dims)
    grad_sq_o, prod_o = gather_quarters(left_quarter(grad_o, left_o), O_DIMS[0])
    grad_sq_q, prod_q = gather_quarters(left_quarter(grad_q, left_q), Q_DIMS[0])
    dir_o = direction_of(prod_o, ro)
    dir_q = direction_of(prod_q, rq)
    sums = jnp.stack([grad_sq_q, grad_sq_o, jnp.sum(dir_q * dir_q), jnp.sum(dir_o * dir_o)])
    sums = jnp.broadcast_to(sums[:, None], (4, 128))
    sums = (sums + other_core(sums))[:, 0]
    scale_q = jnp.sqrt(sums[0] / (sums[2] + 1e-06))
    scale_o = jnp.sqrt(sums[1] / (sums[3] + 1e-06))

    outs = []
    for w, m, base_all, direction, scale in (
        (wq, mq, base_all_q, dir_q, scale_q),
        (wo, mo, base_all_o, dir_o, scale_o),
    ):
        rows = w.shape[0]
        mine = lax.dynamic_slice_in_dim(direction, fs * rows, rows, 0)
        moment = 0.8 * m + scale * mine
        weight = 0.998 * w - 0.02 * moment
        copy = (base_all.astype(F32) - (0.02 * scale) * direction).astype(BF16)
        outs += [weight, moment, copy]
    return tuple(outs)


def solution(mesh):
    grid = Mesh(mesh.devices.reshape(4, 4, 4, 2), AXES)
    tokens = ("z", "x", "y")
    fs = ("z", "x")
    half = [P(tokens, None), P(tokens, "tp"), P(fs, "tp"), P(fs, "tp"), P(fs, None), P("tp", None, None)]
    outs = [P(fs, "tp"), P(fs, "tp"), P(None, "tp")]
    return jax.shard_map(
        local, mesh=grid, in_specs=tuple(half * 2), out_specs=tuple(outs * 2), check_vma=False
    )
```

```python
import functools

import jax
import jax.numpy as jnp
from jax import lax
from jax.experimental import pallas as pl
from jax.experimental.pallas import tpu as pltpu
from jax.sharding import Mesh, PartitionSpec as P

AXES = ("z", "x", "y", "tp")
F32 = jnp.float32
BF16 = jnp.bfloat16
MIB = 1 << 20

SPLIT = ("x", "z")
SECOND = ("y", "x")
THIRD = ("z", "y")
BASE_FIRST = ("z", "x")
BASE_SECOND = ("x", "z")
SHIFTS = (1, 3, 2)


def shift_pairs(dims, k):
    pairs = []
    for z in range(4):
        for x in range(4):
            for y in range(4):
                for t in range(2):
                    at = {"z": z, "x": x, "y": y}
                    at[dims[t]] = (at[dims[t]] + k) % 4
                    there = ((at["z"] * 4 + at["x"]) * 4 + at["y"]) * 2 + t
                    pairs.append((((z * 4 + x) * 4 + y) * 2 + t, there))
    return pairs


def shifted(array, dims, k):
    return lax.ppermute(array, AXES, shift_pairs(dims, k))


def exchanged(blocks, dims):
    got = {k: shifted(blocks[k], dims, k) for k in SHIFTS}
    return [blocks[0], got[1], got[2], got[3]]


def other_core(array):
    return lax.ppermute(array, "tp", [(0, 1), (1, 0)])


def place_on(dims):
    t = lax.axis_index("tp")
    return jnp.where(t == 0, lax.axis_index(dims[0]), lax.axis_index(dims[1]))


def call(body, name, outs, scalars, *arrays, scratch=(), flops=1, vmem=24):
    shapes = [jax.ShapeDtypeStruct(s, d) for s, d in outs]
    bytes_moved = sum(a.size * a.dtype.itemsize for a in arrays)
    return pl.pallas_call(
        body,
        name=name,
        out_shape=shapes,
        in_specs=[pl.BlockSpec(memory_space=pltpu.SMEM)]
        + [pl.BlockSpec(memory_space=pltpu.VMEM)] * len(arrays),
        out_specs=[pl.BlockSpec(memory_space=pltpu.VMEM)] * len(outs),
        scratch_shapes=list(scratch),
        cost_estimate=pl.CostEstimate(
            flops=max(flops, 1), bytes_accessed=bytes_moved, transcendentals=0
        ),
        compiler_params=pltpu.CompilerParams(vmem_limit_bytes=vmem * MIB),
    )(scalars, *arrays)


def partial_body(me_ref, s_ref, u_ref, o0, o1, o2, o3, acc):
    step = pl.program_id(0)
    rows = s_ref.shape[1]
    width = u_ref.shape[1] // 4

    @pl.when(step == 0)
    def _():
        acc[...] = jnp.zeros_like(acc)

    for m in range(rows // 256):
        at = slice(m * 256, (m + 1) * 256)
        acc[at, :] += lax.dot_general(
            s_ref[:, at], u_ref[...], (((0,), (0,)), ((), ())), preferred_element_type=F32
        )

    @pl.when(step == pl.num_programs(0) - 1)
    def _():
        if width % 128 == 0:
            for k, out in enumerate((o0, o1, o2, o3)):
                block = pl.multiple_of((me_ref[0] + k) % 4 * width, 128)
                out[...] = acc[:, pl.ds(block, width)].astype(BF16)
        else:
            for j in range(4):
                value = acc[:, j * width : (j + 1) * width].astype(BF16)
                for k, out in enumerate((o0, o1, o2, o3)):

                    @pl.when((me_ref[0] + k) % 4 == j)
                    def _():
                        out[...] = value


def partial_grad(saved, upstream, me, steps):
    tokens, rows = saved.shape
    cols = upstream.shape[1]
    depth = tokens // steps
    return pl.pallas_call(
        partial_body,
        name="partial_grad",
        grid=(steps,),
        in_specs=[
            pl.BlockSpec(memory_space=pltpu.SMEM),
            pl.BlockSpec((depth, rows), lambda i: (i, 0)),
            pl.BlockSpec((depth, cols), lambda i: (i, 0)),
        ],
        out_specs=[pl.BlockSpec((rows, cols // 4), lambda i: (0, 0))] * 4,
        out_shape=[jax.ShapeDtypeStruct((rows, cols // 4), BF16)] * 4,
        scratch_shapes=[pltpu.VMEM((rows, cols), F32)],
        cost_estimate=pl.CostEstimate(
            flops=2 * tokens * rows * cols,
            bytes_accessed=2 * tokens * (rows + cols),
            transcendentals=0,
        ),
        compiler_params=pltpu.CompilerParams(
            vmem_limit_bytes=24 * MIB, dimension_semantics=("arbitrary",)
        ),
    )(me, saved, upstream)


def four(a, b, c, d):
    f = lambda v: v.astype(F32)
    return (f(a) + f(c)) + (f(b) + f(d))


def first_sum_body(me_ref, p0, p1, p2, p3, q0, q1, q2, q3, *outs):
    for k, out in enumerate(outs):
        block = (me_ref[0] + k) % 4
        at = pl.ds(pl.multiple_of(block * 256, 256), 256)
        out[:256, :] = four(p0[at, :], p1[at, :], p2[at, :], p3[at, :]).astype(BF16)
        at = pl.ds(pl.multiple_of(block * 128, 128), 128)
        out[256:, :192] = four(q0[at, :], q1[at, :], q2[at, :], q3[at, :]).astype(BF16)
        out[256:, 192:] = jnp.zeros((128, 64), BF16)


def sum_body(me_ref, a, b, c, d, out):
    out[...] = four(a[...], b[...], c[...], d[...]).astype(BF16)


def left_body(me_ref, g0, g1, g2, g3, lo, lq, out, grad_o, grad_q):
    for k, g in enumerate((g0, g1, g2, g3)):
        block = (me_ref[0] - k + 4) % 4
        grad_o[pl.ds(pl.multiple_of(block * 256, 256), 256), :] = g[:256, :]
        grad_q[pl.ds(pl.multiple_of(block * 128, 128), 128), :] = g[256:, :]
    tail = jnp.zeros((16, 256), F32)
    row = lax.broadcasted_iota(jnp.int32, (16, 256), 0)
    for n, grad in enumerate((grad_q, grad_o)):
        value = grad[...].astype(F32)
        total = jnp.sum(value * value, axis=(0, 1), keepdims=True)
        high = total.astype(BF16).astype(F32)
        tail = jnp.where(row == 2 * n, high, tail)
        tail = jnp.where(row == 2 * n + 1, total - high, tail)
    out[1536:, :] = tail.astype(BF16)
    for m in range(4):
        at = slice(m * 256, (m + 1) * 256)
        out[at, :] = jnp.dot(lo[at, :], grad_o[...], preferred_element_type=F32).astype(BF16)
    for m in range(2):
        at = slice(m * 256, (m + 1) * 256)
        out[1024 + m * 256 : 1280 + m * 256, :] = jnp.dot(
            lq[at, :], grad_q[...], preferred_element_type=F32
        ).astype(BF16)


def right_body(me_ref, p0, p1, p2, p3, rq, ro, dir_q, dir_o, sums, prod_o, prod_q):
    grads = []
    for k, p in enumerate((p0, p1, p2, p3)):
        block = (me_ref[0] - k + 4) % 4
        prod_o[block] = p[:1024, :]
        prod_q[block] = p[1024:1536, :192]
        tail = p[1536:, :128].astype(F32)
        grads.append([tail[2 * n : 2 * n + 1] + tail[2 * n + 1 : 2 * n + 2] for n in range(2)])
    grad_sq = [(grads[0][n] + grads[2][n]) + (grads[1][n] + grads[3][n]) for n in range(2)]
    dir_sq = []
    for out, prod, right, width in ((dir_q, prod_q, rq, 192), (dir_o, prod_o, ro, 256)):
        total = jnp.zeros((1, 2 * width), F32)
        for n in range(2):
            for m in range(out.shape[0] // 256):
                at = slice(m * 256, (m + 1) * 256)
                value = jnp.dot(
                    prod[2 * n, at, :], right[n, :width, :], preferred_element_type=F32
                ) + jnp.dot(
                    prod[2 * n + 1, at, :], right[n, width:, :], preferred_element_type=F32
                )
                out[at, n * 2 * width : (n + 1) * 2 * width] = value
                total += jnp.sum(value * value, axis=0, keepdims=True)
        dir_sq.append(jnp.sum(total, axis=1, keepdims=True))
    row = lax.broadcasted_iota(jnp.int32, (8, 128), 0)
    value = jnp.zeros((8, 128), F32)
    for n in range(2):
        value = jnp.where(row == n, grad_sq[n], value)
        value = jnp.where(row == 2 + n, dir_sq[n], value)
    sums[...] = value


def packed_body(me_ref, wq, mq, lq, wo, mo, lo, out):
    out[:64, :] = (0.998 * wo[...] - 0.016 * mo[...]).astype(BF16)
    out[64:96, :768] = (0.998 * wq[...] - 0.016 * mq[...]).astype(BF16)
    out[64:96, 768:] = jnp.zeros((32, 256), BF16)
    half = me_ref[0]
    out[96:128, :] = lo[pl.ds(pl.multiple_of(half * 32, 32), 32), :]
    out[128:, :512] = lq[pl.ds(pl.multiple_of(half * 16, 16), 16), :]
    out[128:, 512:] = jnp.zeros((16, 512), BF16)


def factors_body(at_ref, mine, theirs, lo, lq):
    half = at_ref[32]
    for which, pieces in enumerate((mine, theirs)):
        core = half if which == 0 else 1 - half
        for n in range(16):
            row = at_ref[which * 16 + n] * 2 + core
            lo[pl.ds(pl.multiple_of(row * 32, 32), 32), :] = pieces[n // 4, n % 4, :32, :]
            lq[pl.ds(pl.multiple_of(row * 16, 16), 16), :] = pieces[n // 4, n % 4, 32:, :512]


def final_body(at_ref, here, there, dir_q, dir_o, b0, b1, b2, b3, wq, mq, wo, mo,
               new_wq, new_mq, copy_q, new_wo, new_mo, copy_o):
    sums = here[...] + there[...]
    scale_q = jnp.sqrt(sums[0:1, 0:1] / (sums[2:3, 0:1] + 1e-06))
    scale_o = jnp.sqrt(sums[1:2, 0:1] / (sums[3:4, 0:1] + 1e-06))
    fs = at_ref[33]
    for w, m, new_w, new_m, direction, scale, rows in (
        (wq, mq, new_wq, new_mq, dir_q, scale_q, 32),
        (wo, mo, new_wo, new_mo, dir_o, scale_o, 64),
    ):
        mine = direction[pl.ds(pl.multiple_of(fs * rows, 32), rows), :]
        moment = 0.8 * m[...] + scale * mine
        new_m[...] = moment
        new_w[...] = 0.998 * w[...] - 0.02 * moment
    for k, base in enumerate((b0, b1, b2, b3)):
        for n in range(4):
            row = at_ref[4 * k + n]
            at = pl.ds(pl.multiple_of(row * 64, 64), 64)
            copy_o[at, :] = (
                base[n, :64, :].astype(F32) - (0.02 * scale_o) * dir_o[at, :]
            ).astype(BF16)
            at = pl.ds(pl.multiple_of(row * 32, 32), 32)
            copy_q[at, :] = (
                base[n, 64:, :768].astype(F32) - (0.02 * scale_q) * dir_q[at, :]
            ).astype(BF16)


def local(sq, uq, wq, mq, lq, rq, so, uo, wo, mo, lo, ro):
    t = lax.axis_index("tp")
    z, x = lax.axis_index("z"), lax.axis_index("x")
    place = lambda dims: place_on(dims).astype(jnp.int32).reshape(1)
    k2, k1 = jnp.arange(16) // 4, jnp.arange(16) % 4
    order_0 = (z - k1) % 4 * 4 + (x - k2) % 4
    order_1 = (z - k2) % 4 * 4 + (x - k1) % 4
    mine = jnp.where(t == 0, order_0, order_1)
    theirs = jnp.where(t == 0, order_1, order_0)
    table = jnp.concatenate([mine, theirs, jnp.stack([t, z * 4 + x])]).astype(jnp.int32)

    packed = call(
        packed_body, "packed", [((144, 1024), BF16)], t.astype(jnp.int32).reshape(1),
        wq, mq, lq, wo, mo, lo, vmem=4,
    )[0]
    first = exchanged([packed] * 4, BASE_FIRST)

    parts_q = partial_grad(sq, uq, place(SPLIT), 3)
    got_q = exchanged(parts_q, SPLIT)
    parts_o = partial_grad(so, uo, place(SPLIT), 4)
    got_o = exchanged(parts_o, SPLIT)

    base = jnp.stack([p[:96] for p in first])
    factor = jnp.stack([p[96:] for p in first])
    factors = exchanged([factor] * 4, BASE_SECOND)
    factors = jnp.stack(factors)
    left_o, left_q = call(
        factors_body, "factors", [((1024, 1024), BF16), ((512, 512), BF16)], table,
        factors, other_core(factors), vmem=8,
    )

    blocks = call(
        first_sum_body, "first_sum", [((384, 256), BF16)] * 4, place(SECOND), *got_o, *got_q, vmem=8
    )
    got = exchanged(blocks, SECOND)
    value = call(sum_body, "second_sum", [((384, 256), BF16)], place(THIRD), *got, vmem=4)[0]
    bases = exchanged([base] * 4, BASE_SECOND)
    got = exchanged([value] * 4, THIRD)
    value = call(sum_body, "third_sum", [((384, 256), BF16)], place(THIRD), *got, vmem=4)[0]
    got = exchanged([value] * 4, SECOND)
    prod = call(
        left_body, "left", [((1552, 256), BF16)], place(SECOND), *got, left_o, left_q,
        scratch=[pltpu.VMEM((1024, 256), BF16), pltpu.VMEM((512, 256), BF16)],
        flops=2 * 1280 * 1024 * 256, vmem=8,
    )[0]
    got = exchanged([prod] * 4, SPLIT)
    dir_q, dir_o, sums = call(
        right_body, "right", [((512, 768), F32), ((1024, 1024), F32), ((8, 128), F32)],
        place(SPLIT), *got, rq, ro,
        scratch=[pltpu.VMEM((4, 1024, 256), BF16), pltpu.VMEM((4, 512, 192), BF16)],
        flops=2 * 1024 * 1024 * 800, vmem=20,
    )
    return call(
        final_body, "final",
        [(wq.shape, F32), (mq.shape, F32), ((512, 768), BF16),
         (wo.shape, F32), (mo.shape, F32), ((1024, 1024), BF16)],
        table, sums, other_core(sums), dir_q, dir_o, *bases, wq, mq, wo, mo, vmem=20,
    )


def solution(mesh):
    grid = Mesh(mesh.devices.reshape(4, 4, 4, 2), AXES)
    tokens = ("z", "x", "y")
    fs = ("z", "x")
    half = [P(tokens, None), P(tokens, "tp"), P(fs, "tp"), P(fs, "tp"), P(fs, None), P("tp", None, None)]
    outs = [P(fs, "tp"), P(fs, "tp"), P(None, "tp")]
    return jax.shard_map(
        local, mesh=grid, in_specs=tuple(half * 2), out_specs=tuple(outs * 2), check_vma=False
    )
```

```python
import jax
import jax.numpy as jnp
from jax import lax
from jax.experimental import pallas as pl
from jax.experimental.pallas import tpu as pltpu
from jax.sharding import Mesh, PartitionSpec as P


AXES = ("z", "x", "y", "tp")
F32 = jnp.float32
BF16 = jnp.bfloat16
MIB = 1 << 20

SPLIT = ("x", "z")
SECOND = ("y", "x")
THIRD = ("z", "y")
BASE_FIRST = ("z", "x")
BASE_SECOND = ("x", "z")
SHIFTS = (1, 3, 2)


def shift_pairs(dims, k):
    pairs = []
    for z in range(4):
        for x in range(4):
            for y in range(4):
                for t in range(2):
                    at = {"z": z, "x": x, "y": y}
                    at[dims[t]] = (at[dims[t]] + k) % 4
                    there = ((at["z"] * 4 + at["x"]) * 4 + at["y"]) * 2 + t
                    pairs.append((((z * 4 + x) * 4 + y) * 2 + t, there))
    return pairs


def shifted(array, dims, k):
    return lax.ppermute(array, AXES, shift_pairs(dims, k))


def exchanged(blocks, dims):
    got = {}
    for k in SHIFTS:
        got[k] = shifted(blocks[k], dims, k)
    return [blocks[0], got[1], got[2], got[3]]


def other_core(array):
    return lax.ppermute(array, "tp", [(0, 1), (1, 0)])


def place_on(dims):
    t = lax.axis_index("tp")
    return jnp.where(t == 0, lax.axis_index(dims[0]), lax.axis_index(dims[1]))


def call(body, outs, scalars, *arrays, scratch=(), flops=1, vmem=24):
    shapes = [jax.ShapeDtypeStruct(s, d) for s, d in outs]
    bytes_moved = sum(a.size * a.dtype.itemsize for a in arrays)
    return _call(body, shapes, bytes_moved, scalars, arrays, scratch, flops, vmem, outs)


def _call(body, shapes, bytes_moved, scalars, arrays, scratch, flops, vmem, outs):
    return pl.pallas_call(
        body,
        out_shape=shapes,
        in_specs=[pl.BlockSpec(memory_space=pltpu.SMEM)]
        + [pl.BlockSpec(memory_space=pltpu.VMEM)] * len(arrays),
        out_specs=[pl.BlockSpec(memory_space=pltpu.VMEM)] * len(outs),
        scratch_shapes=list(scratch),
        cost_estimate=pl.CostEstimate(
            flops=max(flops, 1), bytes_accessed=bytes_moved, transcendentals=0
        ),
        compiler_params=pltpu.CompilerParams(vmem_limit_bytes=vmem * MIB),
    )(scalars, *arrays)


PIECES = ((0, 512), (512, 1536), (1536, 3072))


def summed_over_tokens(s_hbm, u_hbm, s, u, acc, sems, finish):
    copies = []
    for n, (start, stop) in enumerate(PIECES):
        at = pl.ds(start, stop - start)
        copies.append([
            pltpu.make_async_copy(s_hbm.at[at, :], s.at[at, :], sems.at[n, 0]),
            pltpu.make_async_copy(u_hbm.at[at, :], u.at[at, :], sems.at[n, 1]),
        ])
    for pair in copies:
        for copy in pair:
            copy.start()
    for n, (start, stop) in enumerate(PIECES):
        for copy in copies[n]:
            copy.wait()
        for m in range(acc.shape[0] // 256):
            rows = slice(m * 256, (m + 1) * 256)
            value = lax.dot_general(
                s[start:stop, rows], u[start:stop, :], (((0,), (0,)), ((), ())),
                preferred_element_type=F32,
            )
            value = value if n == 0 else acc[rows, :] + value
            if stop < 3072:
                acc[rows, :] = value
            else:
                finish(rows, value)


def partial_output_body(me_ref, s_hbm, u_hbm, o0, o1, o2, o3, s, u, acc, sems):
    def finish(rows, value):
        acc[rows, :] = value
        for k, out in enumerate((o0, o1, o2, o3)):
            block = pl.multiple_of((me_ref[0] + k) % 4 * 256, 256)
            out[rows, :] = acc[rows, pl.ds(block, 256)].astype(BF16)

    summed_over_tokens(s_hbm, u_hbm, s, u, acc, sems, finish)


def partial_query_body(me_ref, s_hbm, u_hbm, o0, o1, o2, o3, s, u, acc, sems, quarters):
    def finish(rows, value):
        value = value.astype(BF16)
        for n in range(4):
            quarters[n, rows, :] = value[:, n * 192 : (n + 1) * 192]

    summed_over_tokens(s_hbm, u_hbm, s, u, acc, sems, finish)
    for k, out in enumerate((o0, o1, o2, o3)):
        out[...] = quarters[(me_ref[0] + k) % 4]


def partial_grad(body, saved, upstream, me, scratch=()):
    tokens, rows = saved.shape
    cols = upstream.shape[1]
    arrays = in_hbm([saved, upstream])
    return pl.pallas_call(
        body,
        in_specs=[pl.BlockSpec(memory_space=pltpu.SMEM)]
        + [pl.BlockSpec(memory_space=pltpu.HBM)] * 2,
        out_specs=[pl.BlockSpec(memory_space=pltpu.VMEM)] * 4,
        out_shape=[jax.ShapeDtypeStruct((rows, cols // 4), BF16)] * 4,
        scratch_shapes=[pltpu.VMEM(a.shape, BF16) for a in arrays]
        + [pltpu.VMEM((rows, cols), F32), pltpu.SemaphoreType.DMA((3, 2)), *scratch],
        cost_estimate=pl.CostEstimate(
            flops=2 * tokens * rows * cols,
            bytes_accessed=2 * tokens * (rows + cols),
            transcendentals=0,
        ),
        compiler_params=pltpu.CompilerParams(vmem_limit_bytes=28 * MIB),
    )(me, *arrays)


def four(a, b, c, d):
    f = lambda v: v.astype(F32)
    return (f(a) + f(c)) + (f(b) + f(d))


def first_sum_body(me_ref, p0, p1, p2, p3, q0, q1, q2, q3, *outs):
    for k, out in enumerate(outs):
        block = (me_ref[0] + k) % 4
        at = pl.ds(pl.multiple_of(block * 256, 256), 256)
        out[:256, :] = four(p0[at, :], p1[at, :], p2[at, :], p3[at, :]).astype(BF16)
        at = pl.ds(pl.multiple_of(block * 128, 128), 128)
        out[256:, :192] = four(q0[at, :], q1[at, :], q2[at, :], q3[at, :]).astype(BF16)
        out[256:, 192:] = jnp.zeros((128, 64), BF16)


def factor_body(p0, p1, p2, p3, out, sems):
    copies = [
        pltpu.make_async_copy(p.at[:, pl.ds(0, 48), :], out.at[k], sems.at[k])
        for k, p in enumerate((p0, p1, p2, p3))
    ]
    for copy in copies:
        copy.start()
    for copy in copies:
        copy.wait()


def factor_pile(pieces):
    return pl.pallas_call(
        factor_body,
        name="factor",
        in_specs=[pl.BlockSpec(memory_space=pltpu.HBM)] * 4,
        out_specs=pl.BlockSpec(memory_space=pltpu.VMEM),
        out_shape=jax.ShapeDtypeStruct((4, 4, 48, 1024), BF16),
        scratch_shapes=[pltpu.SemaphoreType.DMA((4,))],
        cost_estimate=pl.CostEstimate(
            flops=1, bytes_accessed=4 * 4 * 48 * 1024 * 4, transcendentals=0
        ),
        compiler_params=pltpu.CompilerParams(vmem_limit_bytes=4 * MIB),
    )(*pieces)


def in_hbm(arrays):
    return [pltpu.with_memory_space_constraint(a, pltpu.HBM) for a in arrays]


def base_body(me_ref, p0, p1, p2, p3, out_a, out_b):
    for k, pieces in enumerate((p0, p1, p2, p3)):
        for n in range(4):
            (out_a, out_b)[k // 2][k % 2, n] = pieces[n, 48:, :]


def sum_body(me_ref, a, b, c, d, out):
    out[...] = four(a[...], b[...], c[...], d[...]).astype(BF16)


def left_body(at_ref, g0, g1, g2, g3, first, other, out, grad_o, grad_q, lo, lq):
    for k, g in enumerate((g0, g1, g2, g3)):
        block = (at_ref[32] - k + 4) % 4
        grad_o[pl.ds(pl.multiple_of(block * 256, 256), 256), :] = g[:256, :]
        grad_q[pl.ds(pl.multiple_of(block * 128, 128), 128), :] = g[256:, :]
    core = at_ref[33]
    for n in range(8):
        half, pieces = (core, first) if n < 4 else (1 - core, other)
        for m in range(4):
            row = at_ref[4 * n + m] * 2 + half
            lo[pl.ds(pl.multiple_of(row * 32, 32), 32), :] = pieces[n % 4, m, :32, :]
            lq[pl.ds(pl.multiple_of(row * 16, 16), 16), :] = pieces[n % 4, m, 32:, :512]
    tail = jnp.zeros((16, 256), F32)
    row = lax.broadcasted_iota(jnp.int32, (16, 256), 0)
    for n, grad in enumerate((grad_q, grad_o)):
        value = grad[...].astype(F32)
        total = jnp.sum(value * value, axis=(0, 1), keepdims=True)
        high = total.astype(BF16).astype(F32)
        tail = jnp.where(row == 2 * n, high, tail)
        tail = jnp.where(row == 2 * n + 1, total - high, tail)
    out[1536:, :] = tail.astype(BF16)
    for m in range(4):
        at = slice(m * 256, (m + 1) * 256)
        out[at, :] = jnp.dot(lo[at, :], grad_o[...], preferred_element_type=F32).astype(BF16)
    for m in range(2):
        at = slice(m * 256, (m + 1) * 256)
        out[1024 + m * 256 : 1280 + m * 256, :] = jnp.dot(
            lq[at, :], grad_q[...], preferred_element_type=F32
        ).astype(BF16)


def right_body(me_ref, p0, p1, p2, p3, rq, ro, dir_q, dir_o, sums, prod_o, prod_q):
    grads = []
    for k, p in enumerate((p0, p1, p2, p3)):
        block = (me_ref[0] - k + 4) % 4
        prod_o[block] = p[:1024, :]
        prod_q[block] = p[1024:1536, :192]
        tail = p[1536:, :128].astype(F32)
        grads.append([tail[2 * n : 2 * n + 1] + tail[2 * n + 1 : 2 * n + 2] for n in range(2)])
    grad_sq = [(grads[0][n] + grads[2][n]) + (grads[1][n] + grads[3][n]) for n in range(2)]
    dir_sq = []
    for out, prod, right, width in ((dir_q, prod_q, rq, 192), (dir_o, prod_o, ro, 256)):
        total = jnp.zeros((1, 2 * width), F32)
        for n in range(2):
            for m in range(out.shape[0] // 256):
                at = slice(m * 256, (m + 1) * 256)
                value = jnp.dot(
                    prod[2 * n, at, :], right[n, :width, :], preferred_element_type=F32
                ) + jnp.dot(
                    prod[2 * n + 1, at, :], right[n, width:, :], preferred_element_type=F32
                )
                out[at, n * 2 * width : (n + 1) * 2 * width] = value
                total += jnp.sum(value * value, axis=0, keepdims=True)
        dir_sq.append(jnp.sum(total, axis=1, keepdims=True))
    row = lax.broadcasted_iota(jnp.int32, (8, 128), 0)
    value = jnp.zeros((8, 128), F32)
    for n in range(2):
        value = jnp.where(row == n, grad_sq[n], value)
        value = jnp.where(row == 2 + n, dir_sq[n], value)
    sums[...] = value


def packed_body(me_ref, wq, mq, lq, wo, mo, lo, out):
    core, odd = me_ref[0], me_ref[1]
    out[:32, :] = lo[pl.ds(pl.multiple_of(core * 32, 32), 32), :]
    out[32:48, :512] = lq[pl.ds(pl.multiple_of(core * 16, 16), 16), :]
    out[32:48, 512:] = jnp.zeros((16, 512), BF16)
    at = pl.ds(pl.multiple_of(odd * 512, 512), 512)
    base = (0.998 * wo[:, at] - 0.016 * mo[:, at]).astype(BF16)
    out[48:, :512] = base[:48, :]
    out[48:64, 512:] = base[48:, :]
    at = pl.ds(pl.multiple_of(odd * 384, 128), 384)
    out[64:, 512:896] = (0.998 * wq[:, at] - 0.016 * mq[:, at]).astype(BF16)
    out[64:, 896:] = jnp.zeros((32, 128), BF16)


def pieces_body(me_ref, a, b, c, d, out):
    for k, part in enumerate((a, b, c, d)):
        out[k] = part[...]


def final_body(at_ref, here, there, dir_q, dir_o, a0, a1, b0, b1, wq, mq, wo, mo,
               new_wq, new_mq, copy_q, new_wo, new_mo, copy_o):
    sums = here[...] + there[...]
    scale_q = jnp.sqrt(sums[0:1, 0:1] / (sums[2:3, 0:1] + 1e-06))
    scale_o = jnp.sqrt(sums[1:2, 0:1] / (sums[3:4, 0:1] + 1e-06))
    fs, odd = at_ref[34], at_ref[35]
    for w, m, new_w, new_m, direction, scale, rows in (
        (wq, mq, new_wq, new_mq, dir_q, scale_q, 32),
        (wo, mo, new_wo, new_mo, dir_o, scale_o, 64),
    ):
        mine = direction[pl.ds(pl.multiple_of(fs * rows, 32), rows), :]
        moment = 0.8 * m[...] + scale * mine
        new_m[...] = moment
        new_w[...] = 0.998 * w[...] - 0.02 * moment
    for k in range(8):
        pieces = (a0, a1, b0, b1)[k // 2]
        half = odd if k < 4 else 1 - odd
        at_o = pl.ds(pl.multiple_of(half * 512, 512), 512)
        at_q = pl.ds(pl.multiple_of(half * 384, 128), 384)
        for n in range(4):
            row = at_ref[4 * (k % 4) + n]
            for start, part in (
                (0, pieces[k % 2, n, :, :512]), (48, pieces[k % 2, n, :16, 512:])
            ):
                rows = pl.ds(pl.multiple_of(row * 64 + start, 16), part.shape[0])
                copy_o[rows, at_o] = (
                    part.astype(F32) - (0.02 * scale_o) * dir_o[rows, at_o]
                ).astype(BF16)
            rows = pl.ds(pl.multiple_of(row * 32, 32), 32)
            copy_q[rows, at_q] = (
                pieces[k % 2, n, 16:, 512:896].astype(F32) - (0.02 * scale_q) * dir_q[rows, at_q]
            ).astype(BF16)


def step(sq, uq, wq, mq, lq, rq, so, uo, wo, mo, lo, ro):
    numbers = lambda *values: jnp.stack(values).astype(jnp.int32)
    t = lax.axis_index("tp")
    z, x = lax.axis_index("z"), lax.axis_index("x")
    odd = lax.axis_index("y") % 2
    me = numbers(place_on(SPLIT))
    k2, k1 = jnp.arange(16) // 4, jnp.arange(16) % 4
    order_0 = (z - k1) % 4 * 4 + (x - k2) % 4
    order_1 = (z - k2) % 4 * 4 + (x - k1) % 4
    mine = jnp.where(t == 0, order_0, order_1)
    theirs = jnp.where(t == 0, order_1, order_0)
    second = place_on(SECOND)
    table = jnp.concatenate([mine, theirs, jnp.stack([second, t, z * 4 + x, odd])]).astype(jnp.int32)

    parts_o = partial_grad(partial_output_body, so, uo, me)
    got_o = exchanged(parts_o, SPLIT)
    packed = call(
        packed_body, [((96, 1024), BF16)], numbers(t, odd), wq, mq, lq, wo, mo, lo, vmem=4
    )[0]
    first = exchanged([packed] * 4, BASE_FIRST)
    parts_q = partial_grad(partial_query_body, sq, uq, me, [pltpu.VMEM((4, 512, 192), BF16)])
    got_q = exchanged(parts_q, SPLIT)
    pieces = call(pieces_body, [((4, 96, 1024), BF16)], me, *first, vmem=4)[0]
    pieces = exchanged([pieces] * 4, BASE_SECOND)

    blocks = call(first_sum_body, [((384, 256), BF16)] * 4, numbers(second), *got_o, *got_q, vmem=8)
    got = exchanged(blocks, SECOND)
    value = call(sum_body, [((384, 256), BF16)], me, *got, vmem=4)[0]
    got = exchanged([value] * 4, THIRD)
    value = call(sum_body, [((384, 256), BF16)], me, *got, vmem=4)[0]
    got = exchanged([value] * 4, SECOND)
    pieces = in_hbm(pieces)
    factor = factor_pile(pieces)
    factor_else = other_core(factor)
    prod = call(
        left_body, [((1552, 256), BF16)], table, *got, factor, factor_else,
        scratch=[
            pltpu.VMEM((1024, 256), BF16), pltpu.VMEM((512, 256), BF16),
            pltpu.VMEM((1024, 1024), BF16), pltpu.VMEM((512, 512), BF16),
        ],
        flops=2 * 1280 * 1024 * 256, vmem=16,
    )[0]
    got = exchanged([prod] * 4, SPLIT)
    base_a, base_b = call(base_body, [((2, 4, 48, 1024), BF16)] * 2, me, *pieces, vmem=8)
    else_a = shifted(base_a, ("y", "y"), 1)
    else_b = shifted(base_b, ("y", "y"), 3)
    dir_q, dir_o, sums = call(
        right_body, [((512, 768), F32), ((1024, 1024), F32), ((8, 128), F32)],
        me, *got, rq, ro,
        scratch=[pltpu.VMEM((4, 1024, 256), BF16), pltpu.VMEM((4, 512, 192), BF16)],
        flops=2 * 1024 * 1024 * 800, vmem=20,
    )
    return call(
        final_body,
        [(wq.shape, F32), (mq.shape, F32), ((512, 768), BF16),
         (wo.shape, F32), (mo.shape, F32), ((1024, 1024), BF16)],
        table, sums, other_core(sums), dir_q, dir_o, base_a, base_b, else_a, else_b,
        wq, mq, wo, mo, vmem=24,
    )


def solution(mesh):
    grid = Mesh(mesh.devices.reshape(4, 4, 4, 2), AXES)
    tokens = ("z", "x", "y")
    fs = ("z", "x")
    half = [P(tokens, None), P(tokens, "tp"), P(fs, "tp"), P(fs, "tp"), P(fs, None), P("tp", None, None)]
    outs = [P(fs, "tp"), P(fs, "tp"), P(None, "tp")]
    return jax.shard_map(
        step, mesh=grid, in_specs=tuple(half * 2), out_specs=tuple(outs * 2), check_vma=False
    )
```
